32 devices in a mesh: grp: 2 (over y), tp: 4 (over z), dp: 4 (over x, core).
Axes of the slice: x: 2, y: 2, z: 4, core: 2. Of those that a mesh axis runs over, the one named last changes fastest.
Arguments:
- residual_slot_vectors: bfloat16 [128, 4, 4096], P('grp', None, 'dp'), parts along dimension 0, may hold values from -25 to 25
- active_counts: int32 [128], P(('grp', 'dp')), parts along dimension 0, may hold values from 1 to 4, 96 in all
- lookup_map: bfloat16 [2, 4096, 4096], P(None, 'dp', 'tp'), may hold values from -0.09375 to 0.09375
- address_map: bfloat16 [2, 4096, 4096], P(None, 'dp', 'tp'), may hold values from -0.09375 to 0.09375
- content_map: bfloat16 [2, 4096, 4096], P(None, 'dp', 'tp'), may hold values from -0.09375 to 0.09375
- result_valve_map: bfloat16 [2, 4096, 4096], P(None, 'dp', 'tp'), may hold values from -0.09375 to 0.09375
- fading_map_coefficients: bfloat16 [2, 4096, 64], replicated, may hold values from -0.09375 to 0.09375
- writing_intensity_map: bfloat16 [2, 4096, 64], replicated, may hold values from -0.09375 to 0.09375
- result_map: bfloat16 [2, 4096, 4096], P(None, 'tp', 'dp'), may hold values from -0.09375 to 0.09375
- fading_speed_exponent: float32 [2, 64], P(None, 'tp'), may hold values from 0 to 2.3
- fading_bias: float32 [2, 64], P(None, 'tp'), may hold values from -5 to -1
- entry_scaling: bfloat16 [2, 4096], P(None, 'dp'), may hold values from 0.099609375 to 1.8984375
- per_channel_scaling: bfloat16 [2, 64], replicated, may hold values from 0.099609375 to 1.8984375
- extra_shrink_exponent: float32 [2, 128, 4, 64], P(None, ('grp', 'dp'), None, 'tp'), parts along dimension 1, may hold values from -0.7 to 0
- memory_tensors: float32 [2, 128, 64, 4096], P(None, ('grp', 'dp'), None, 'tp'), parts along dimension 1, may hold values from -0.6 to 0.6
Outputs:
- mixed_tokens: bfloat16 [128, 4, 4096], P('grp', None, 'dp'), parts along dimension 0
- new_states: float32 [2, 128, 64, 4096], P(None, ('grp', 'dp'), None, 'tp'), parts along dimension 1
The draws below stay inside these ranges and needn't reach their ends.
There are 2 independent parts, one for each index of `grp`. The reference program is written for one: setup_inputs(seed, part) draws one part's arguments, and reference() takes and returns one part's arrays. A program takes and returns all parts, laid end to end along the dimension named above; an argument that names none is the same for every part. Nothing has to cross between parts.
Inputs may be any that keep to these rules, and one draw needn't show every extreme that they name: `active_counts`: every sequence has at least one live slot, at least one sequence has 4.
All inputs are finite; a program needn't handle non-finite values. No bound on the sum of `active_counts` on one device may be relied on, other than what follows from the above.
Results may differ from the reference program's by a relative error of at most 0.018.
Values may be sent and summed in bfloat16 or wider, within the bound.
A program may use at most 128 MiB of HBM per device.

```python
import math
import jax
import jax.numpy as jnp
import numpy as np
from jax import lax

D = 4096
HEADS = 64
HEAD = 64
BLOCKS = 2
NEW = 4
SEQS = 64
N_DP = 4


def draw_residual_slot_vectors(key, part):
    base_key, column_key = jax.random.split(jax.random.fold_in(key, 11), 2)
    column = jnp.arange(D, dtype=jnp.float32) / D
    rough = jnp.exp(jax.random.uniform(column_key, (D,), jnp.float32, -0.35, 0.35))
    scale = 0.5 * jnp.exp(column * math.log(6.0)) * rough
    values = jax.random.truncated_normal(base_key, -4.0, 4.0, (SEQS, NEW, D), jnp.float32)
    return (values * scale).astype(jnp.bfloat16)


def draw_extra_shrink_exponent(key, part):
    hit_key, depth_key = jax.random.split(jax.random.fold_in(key, 23))
    shape = (BLOCKS, SEQS, NEW, HEADS)
    hits = jax.random.bernoulli(hit_key, 0.1, shape)
    depth = jax.random.uniform(depth_key, shape, jnp.float32, -0.7, -0.22)
    return jnp.where(hits, depth, 0.0).astype(jnp.float32)


def block_scale(own_key, extent, shards, low, largest):
    def one(dim, parts):
        steps = jax.random.uniform(jax.random.fold_in(jax.random.fold_in(own_key, 6), dim), (parts,), jnp.float32, low / len(shards), largest / len(shards))
        return jnp.repeat(jnp.exp(steps), extent[dim] // parts).reshape((-1,) + (1,) * (len(extent) - dim - 1))

    gain = one(*shards[0])
    for cut in shards[1:]:
        gain = gain * one(*cut)
    return gain


def length_profile(count, total, most, lean):
    weights = [(1 << 20) // math.isqrt(rank ** lean) + 1 for rank in range(2, count + 1)]
    spare, holding = total - most - (count - 1), [1] * (count - 1)
    while spare > 0:
        candidates = [i for i in range(count - 1) if holding[i] < most]
        mass, left = sum([weights[i] for i in candidates]), spare
        for i in candidates:
            extra = min(most - holding[i], max(1, left * weights[i] // mass), spare)
            holding[i] = holding[i] + extra
            spare = spare - extra
    return np.array([most] + holding)


def ragged_sizes(rng, count, total, most, skew):
    if count == 2:
        one = jax.random.randint(rng, (), max(1, total - most), min(most, total - 1) + 1)
        return jnp.stack([one, total - one])
    tallies = jnp.asarray(length_profile(count, total, most, skew), jnp.int32)
    couples = (count - 1) // 2
    source_of, receiver = tallies[1:1 + 2 * couples:2], tallies[2:2 + 2 * couples:2]
    slack = jnp.minimum(source_of - 1, most - receiver)
    moved = jax.random.randint(jax.random.fold_in(rng, 1), (couples,), 0, 1 << 20) % (slack + 1)
    tallies = tallies.at[1:1 + 2 * couples:2].set(source_of - moved).at[2:2 + 2 * couples:2].set(receiver + moved)
    return tallies[jax.random.permutation(jax.random.fold_in(rng, 2), count)]


def scatter_about(key, extent, scale, most, cuts=(), kind=jnp.bfloat16):
    gain = block_scale(key, extent, cuts, -0.22, 0.18) if cuts else 1.0
    drawn = jax.random.normal(key, extent, jnp.float32) * scale * gain
    return jnp.minimum(jnp.maximum(drawn, -most), most).astype(kind)


def setup_inputs(seed: int = 0, part: int = 0) -> dict:
    splits = jax.random.split(jax.random.key(seed), 16)
    part_splits = jax.random.split(jax.random.fold_in(splits[15], part), 16)
    residual_slot_vectors = draw_residual_slot_vectors(jax.random.fold_in(jax.random.fold_in(splits[15], part), 71), part)
    active_counts = ragged_sizes(part_splits[1], SEQS, SEQS * 3 // 2, NEW, 1).astype(jnp.int32)
    lookup_map = scatter_about(splits[2], (BLOCKS, D, HEADS * HEAD), D ** -0.5, 0.09375, ((1, 4), (2, 4)))
    address_map = scatter_about(splits[3], (BLOCKS, D, HEADS * HEAD), D ** -0.5, 0.09375, ((1, 4), (2, 4)))
    content_map = scatter_about(splits[4], (BLOCKS, D, HEADS * HEAD), D ** -0.5, 0.09375, ((1, 4), (2, 4)))
    result_valve_map = scatter_about(splits[5], (BLOCKS, D, HEADS * HEAD), D ** -0.5, 0.09375, ((1, 4), (2, 4)))
    fading_map_coefficients = scatter_about(splits[6], (BLOCKS, D, HEADS), D ** -0.5, 0.09375)
    writing_intensity_map = scatter_about(splits[7], (BLOCKS, D, HEADS), D ** -0.5, 0.09375)
    result_map = scatter_about(splits[8], (BLOCKS, HEADS * HEAD, D), (HEADS * HEAD) ** -0.5, 0.09375, ((1, 4), (2, 4)))
    fading_speed_exponent = jnp.clip(2.3 * jax.random.uniform(splits[9], (BLOCKS, HEADS), jnp.float32) ** block_scale(splits[9], (BLOCKS, HEADS), ((1, 4),), -0.2, 0.2), 0.0, 2.3)
    fading_bias = jnp.clip(-5.0 + 4.0 * jax.random.uniform(splits[10], (BLOCKS, HEADS), jnp.float32) ** block_scale(splits[10], (BLOCKS, HEADS), ((1, 4),), -0.2, 0.2), -5.0, -1.0)
    entry_scaling = jnp.clip(1.0 + 0.18 * jax.random.normal(splits[11], (BLOCKS, D), jnp.float32), 0.099609375, 1.8984375).astype(jnp.bfloat16)
    per_channel_scaling = jnp.clip(1.0 + 0.18 * jax.random.normal(splits[12], (BLOCKS, HEAD), jnp.float32), 0.099609375, 1.8984375).astype(jnp.bfloat16)
    extra_shrink_exponent = draw_extra_shrink_exponent(jax.random.fold_in(jax.random.fold_in(splits[15], part), 71), part)
    memory_tensors = scatter_about(part_splits[14], (BLOCKS, SEQS, HEAD, HEADS * HEAD), 0.1, 0.6, ((1, 4), (3, 4)), jnp.float32)
    return dict(residual_slot_vectors=residual_slot_vectors, active_counts=active_counts, lookup_map=lookup_map, address_map=address_map, content_map=content_map, result_valve_map=result_valve_map, fading_map_coefficients=fading_map_coefficients, writing_intensity_map=writing_intensity_map, result_map=result_map, fading_speed_exponent=fading_speed_exponent, fading_bias=fading_bias, entry_scaling=entry_scaling, per_channel_scaling=per_channel_scaling, extra_shrink_exponent=extra_shrink_exponent, memory_tensors=memory_tensors)


EPS = 1e-06

def unit_rows(values):
    return values * lax.rsqrt(lax.optimization_barrier(jnp.sum(values * values, axis=-1, keepdims=True)) + EPS)

def recur(query, keyvec, value, fading_multiplier, beta, live, state):
    reads = []
    for step in range(query.shape[1]):
        decayed = state * jnp.exp(fading_multiplier[:, step])[:, None, :, None]
        guess = jnp.einsum('skhe,shk->she', decayed, keyvec[:, step], precision=lax.Precision.HIGHEST)
        fresh = beta[:, step][..., None] * (value[:, step] - guess)
        updated = decayed + jnp.einsum('shk,she->skhe', keyvec[:, step], fresh, precision=lax.Precision.HIGHEST)
        read = jnp.einsum('skhe,shk->she', updated, query[:, step], precision=lax.Precision.HIGHEST)
        alive = live[:, step]
        state = jnp.where(alive[:, None, None, None], updated, state)
        reads.append(jnp.where(alive[:, None, None], read, 0.0))
    return (jnp.stack(reads, axis=1), state)

def reference(residual_slot_vectors, active_counts, lookup_map, address_map, content_map, result_valve_map, fading_map_coefficients, writing_intensity_map, result_map, fading_speed_exponent, fading_bias, entry_scaling, per_channel_scaling, extra_shrink_exponent, memory_tensors):
    rows = SEQS * NEW
    width = HEADS * HEAD
    resid = residual_slot_vectors.reshape(rows, D)
    position = lax.broadcasted_iota(jnp.int32, (SEQS, NEW), 1)
    live = position < active_counts.astype(jnp.int32)[:, None]
    fresh_states = []
    for block_coefficients in range(BLOCKS):
        widened = resid.astype(jnp.float32)
        factor = lax.rsqrt(lax.optimization_barrier(jnp.sum(widened * widened, axis=1)) / D + EPS)
        scaled = (widened * entry_scaling[block_coefficients].astype(jnp.float32)).astype(jnp.bfloat16)
        pieces = scaled.reshape(rows, N_DP, D // N_DP).astype(jnp.float32)

        def split_product(weight):
            blocked = weight.reshape(N_DP, D // N_DP, weight.shape[1]).astype(jnp.float32)
            part = jnp.einsum('rnd,ndc->nrc', pieces, blocked).astype(jnp.bfloat16)
            part = lax.optimization_barrier(part)
            return lax.optimization_barrier(jnp.sum(part.astype(jnp.float32), axis=0)) * factor[:, None]
        proj_q = split_product(lookup_map[block_coefficients])
        proj_k = split_product(address_map[block_coefficients])
        proj_v = split_product(content_map[block_coefficients])
        proj_z = split_product(result_valve_map[block_coefficients])
        fading_mapped = split_product(fading_map_coefficients[block_coefficients]).reshape(SEQS, NEW, HEADS)
        proj_b = split_product(writing_intensity_map[block_coefficients]).reshape(SEQS, NEW, HEADS)
        query = unit_rows(jax.nn.silu(proj_q).reshape(SEQS, NEW, HEADS, HEAD)) * HEAD ** (-0.5)
        keyvec = unit_rows(jax.nn.silu(proj_k).reshape(SEQS, NEW, HEADS, HEAD))
        value = jax.nn.silu(proj_v).reshape(SEQS, NEW, HEADS, HEAD)
        fading_multiplier = -jnp.exp(fading_speed_exponent[block_coefficients]) * jax.nn.softplus(fading_mapped + fading_bias[block_coefficients]) + extra_shrink_exponent[block_coefficients]
        beta = jax.nn.sigmoid(proj_b)
        state = memory_tensors[block_coefficients].reshape(SEQS, HEAD, HEADS, HEAD)
        reads, state = recur(query, keyvec, value, fading_multiplier, beta, live, state)
        fresh_states.append(state.reshape(SEQS, HEAD, width))
        normed = reads * lax.rsqrt(lax.optimization_barrier(jnp.mean(reads * reads, axis=-1, keepdims=True)) + EPS)
        normed = normed * per_channel_scaling[block_coefficients].astype(jnp.float32)
        gated = (normed.reshape(rows, width) * jax.nn.silu(proj_z)).astype(jnp.bfloat16)
        mixed = jnp.dot(gated, result_map[block_coefficients], preferred_element_type=jnp.float32)
        resid = (resid.astype(jnp.float32) + mixed).astype(jnp.bfloat16)
    return (resid.reshape(SEQS, NEW, D), jnp.stack(fresh_states))
```

```python
import functools

import jax
import jax.numpy as jnp
from jax import lax
from jax.experimental import pallas as pl
from jax.experimental.pallas import tpu as pltpu
from jax.sharding import PartitionSpec as P

BLOCKS = 2
EPS = 1e-06
F32 = jnp.float32
BF16 = jnp.bfloat16
MESH = pl.DeviceIdType.MESH
VMEM = pl.BlockSpec(memory_space=pltpu.VMEM)


def greet(axis, peers):
    barrier = pltpu.get_barrier_semaphore()
    for peer in peers:
        pl.semaphore_signal(barrier, inc=1, device_id={axis: peer}, device_id_type=MESH)
    pl.semaphore_wait(barrier, len(peers))


def send(src, dst, send_sem, recv_sem, axis, peer):
    copy = pltpu.make_async_remote_copy(
        src_ref=src,
        dst_ref=dst,
        send_sem=send_sem,
        recv_sem=recv_sem,
        device_id={axis: peer},
        device_id_type=MESH,
    )
    copy.start()
    return copy


def params(cid):
    return pltpu.CompilerParams(
        collective_id=cid, has_side_effects=True, vmem_limit_bytes=48 * 1024 * 1024
    )


def gather_kernel(n, x_ref, o_ref, land, send_sem, recv_sem):
    me = lax.axis_index("dp")
    peers = [lax.rem(me + d, n) for d in range(1, n)]
    greet("dp", peers)
    copies = [
        send(x_ref, land.at[me], send_sem.at[d], recv_sem.at[d], "dp", peer)
        for d, peer in enumerate(peers)
    ]
    for copy in copies:
        copy.wait()
    o_ref[...] = land[...]
    o_ref[me] = x_ref[...]


def gather_counts(counts, n, cid):
    own = counts.shape[0]
    block = jnp.broadcast_to(jnp.pad(counts, (0, 128 - own))[None, :], (8, 128))
    out = pl.pallas_call(
        functools.partial(gather_kernel, n),
        out_shape=jax.ShapeDtypeStruct((n, 8, 128), jnp.int32),
        in_specs=[VMEM],
        out_specs=VMEM,
        scratch_shapes=[
            pltpu.VMEM((n, 8, 128), jnp.int32),
            pltpu.SemaphoreType.DMA((n - 1,)),
            pltpu.SemaphoreType.DMA((n - 1,)),
        ],
        compiler_params=params(cid),
        name="gather_counts",
    )(block)
    return out[:, 0, :own].reshape(n * own)


def reduce_over_dp(n, x_refs, o_refs, scratch, sems):
    me = lax.axis_index("dp")
    chips = n // 2
    core = lax.rem(me, 2)
    partner = me + 1 - 2 * core
    others = [lax.rem(me + 2 * d, n) for d in range(1, chips)]
    greet("dp", [partner] + others)
    send_sem, recv_sem = sems
    width = chips + 1
    rows = x_refs[0].shape[0] // 2
    mine = pl.multiple_of(core * rows, 16)
    theirs = pl.multiple_of((1 - core) * rows, 16)
    first = []
    for a, x in enumerate(x_refs):
        half = scratch[a][0]
        first.append(
            send(x.at[pl.ds(theirs, rows)], half, send_sem.at[a * width], recv_sem.at[a * width], "dp", partner)
        )
    second = []
    for a, x in enumerate(x_refs):
        half, own, land, back = scratch[a]
        first[a].wait()
        for r in range(0, rows, 16):
            chunk = x[pl.ds(pl.multiple_of(mine + r, 16), 16), :].astype(F32) + half[pl.ds(r, 16), :].astype(F32)
            own[pl.ds(r, 16), :] = chunk.astype(BF16)
        second.append(
            [
                send(own, land.at[d], send_sem.at[a * width + 1 + d], recv_sem.at[a * width + 1 + d], "dp", peer)
                for d, peer in enumerate(others)
            ]
        )
    third = []
    for a, o in enumerate(o_refs):
        half, own, land, back = scratch[a]
        for copy in second[a]:
            copy.wait()
        for r in range(0, rows, 16):
            total = own[pl.ds(r, 16), :].astype(F32)
            for d in range(chips - 1):
                total = total + land[d, pl.ds(r, 16), :].astype(F32)
            own[pl.ds(r, 16), :] = total.astype(BF16)
        slot = a * width + chips
        third.append(send(own, back, send_sem.at[slot], recv_sem.at[slot], "dp", partner))
    for a, o in enumerate(o_refs):
        half, own, land, back = scratch[a]
        o[pl.ds(mine, rows), :] = own[...]
        third[a].wait()
        o[pl.ds(theirs, rows), :] = back[...]


def reduce_scratch(n, shapes):
    out = []
    for rows, cols in shapes:
        half = (rows // 2, cols)
        out += [
            pltpu.VMEM(half, BF16),
            pltpu.VMEM(half, BF16),
            pltpu.VMEM((n // 2 - 1,) + half, BF16),
            pltpu.VMEM(half, BF16),
        ]
    count = len(shapes) * (n // 2 + 1)
    return out + [pltpu.SemaphoreType.DMA((count,)), pltpu.SemaphoreType.DMA((count,))]


def dp_kernel(n, main, small, out_main, out_small, *rest):
    scratch = [rest[0:4], rest[4:8]]
    reduce_over_dp(n, [main, small], [out_main, out_small], scratch, rest[8:10])


def sum_projections(main, small, n, cid):
    shapes = [main.shape, small.shape]
    return pl.pallas_call(
        functools.partial(dp_kernel, n),
        out_shape=[jax.ShapeDtypeStruct(s, BF16) for s in shapes],
        in_specs=[VMEM, VMEM],
        out_specs=[VMEM, VMEM],
        scratch_shapes=reduce_scratch(n, shapes),
        compiler_params=params(cid),
        name="sum_projections",
    )(main, small)


def proj_kernel(where, h, gain, wq, wk, wv, wz, wa, wb, main, small, scaled):
    @pl.when(pl.program_id(0) == 0)
    def _():
        rows = h[...]
        bent = (rows * gain[...].astype(F32)).astype(BF16)
        scaled[...] = bent
        heads = wa.shape[2]
        both = jnp.concatenate([wa[0], wb[0]], axis=1)
        small[:, : 2 * heads] = jnp.dot(bent, both, preferred_element_type=F32).astype(BF16)
        squares = jnp.sum(rows * rows, axis=1, keepdims=True)
        rest = small.shape[1] - 2 * heads
        small[:, 2 * heads :] = jnp.broadcast_to(squares, (rows.shape[0], rest)).astype(BF16)

    tile = wq.shape[2]
    for i, w in enumerate((wq, wk, wv, wz)):
        main[:, i * tile : (i + 1) * tile] = jnp.dot(
            scaled[...], w[0], preferred_element_type=F32
        ).astype(BF16)


def project(h, gain, weights, wa, wb, layer, where):
    rows, feat = h.shape
    cols = weights[0].shape[2]
    tile = min(256, cols)
    heads = wa.shape[2]
    wide = pl.BlockSpec((1, feat, tile), lambda j, s: (layer, 0, j))
    thin = pl.BlockSpec((1, feat, heads), lambda j, s: (layer, s[0], 0))
    return pl.pallas_call(
        proj_kernel,
        out_shape=[
            jax.ShapeDtypeStruct((rows, 4 * cols), BF16),
            jax.ShapeDtypeStruct((rows, 2 * heads + 128), BF16),
        ],
        grid_spec=pltpu.PrefetchScalarGridSpec(
            num_scalar_prefetch=1,
            grid=(cols // tile,),
            in_specs=[
                pl.BlockSpec((rows, feat), lambda j, s: (0, 0)),
                pl.BlockSpec((1, feat), lambda j, s: (0, 0)),
                wide, wide, wide, wide, thin, thin,
            ],
            out_specs=[
                pl.BlockSpec((rows, 4 * tile), lambda j, s: (0, j)),
                pl.BlockSpec((rows, 2 * heads + 128), lambda j, s: (0, 0)),
            ],
            scratch_shapes=[pltpu.VMEM((rows, feat), BF16)],
        ),
        name="project",
    )(where, h, gain, *weights, wa, wb)


def recur_kernel(
    width, size, head_size, heads_all, counts, where, main, small, pos_col, pos_row, speed, bias,
    shrink, gain, state, carried, y, new, q_s, k_s, v_s, z_s, dec_s, beta_s, o_s,
):
    seq = pl.program_id(0)
    slots = q_s.shape[0] // pl.num_programs(0)
    tile = min(256, q_s.shape[1])
    cols = q_s.shape[1]
    row = lax.broadcasted_iota(jnp.int32, (tile, tile), 0) // head_size
    col = lax.broadcasted_iota(jnp.int32, (tile, tile), 1) // head_size
    blocks = (row == col).astype(BF16)

    @pl.when(seq == 0)
    def _():
        own = q_s.shape[0]
        packed = main.shape[0]
        pick = (pos_col[...] == lax.broadcasted_iota(jnp.int32, (own, packed), 1)).astype(BF16)
        few = jnp.dot(pick, small[...], preferred_element_type=F32)
        factor = lax.rsqrt(few[:, 2 * heads_all : 2 * heads_all + 1] / width + EPS)
        heads = speed.shape[1]
        first = where[1] * heads
        ones = lax.broadcasted_iota(jnp.int32, (heads_all, cols), 0)
        lane = lax.broadcasted_iota(jnp.int32, (heads_all, cols), 1) // head_size
        spread_all = (ones == lane + first).astype(BF16)
        spread = (
            lax.broadcasted_iota(jnp.int32, (heads, cols), 0)
            == lax.broadcasted_iota(jnp.int32, (heads, cols), 1) // head_size
        ).astype(F32)
        pa = jnp.dot(few[:, :heads_all].astype(BF16), spread_all, preferred_element_type=F32) * factor
        pb = jnp.dot(
            few[:, heads_all : 2 * heads_all].astype(BF16), spread_all, preferred_element_type=F32
        ) * factor
        exact = functools.partial(
            jnp.dot, precision=lax.Precision.HIGHEST, preferred_element_type=F32
        )
        rate = exact(jnp.broadcast_to(jnp.exp(speed[...]), (8, heads)), spread)[:1]
        offset = exact(jnp.broadcast_to(bias[...], (8, heads)), spread)[:1]
        extra = exact(shrink[...], spread)
        arg = pa + offset
        soft = jnp.maximum(arg, 0.0) + jnp.log1p(jnp.exp(-jnp.abs(arg)))
        dec_s[...] = jnp.exp(extra - rate * soft)
        beta_s[...] = jax.nn.sigmoid(pb)
        for j in range(cols // tile):
            here = slice(j * tile, (j + 1) * tile)
            chunk = jnp.dot(
                pick, main[:, j * 4 * tile : (j + 1) * 4 * tile], preferred_element_type=F32
            ) * factor
            for i, dst in enumerate((q_s, k_s, v_s, z_s)):
                val = chunk[:, i * tile : (i + 1) * tile]
                val = val * jax.nn.sigmoid(val)
                if i < 2:
                    total = jnp.dot((val * val).astype(BF16), blocks, preferred_element_type=F32)
                    val = val * lax.rsqrt(total + EPS)
                    if i == 0:
                        val = val * head_size ** (-0.5)
                dst[:, here] = val
        o_s[...] = jnp.zeros_like(o_s)

    new[...] = state[...]
    key_row = lax.broadcasted_iota(jnp.int32, (size, tile), 0)
    key_col = lax.rem(lax.broadcasted_iota(jnp.int32, (size, tile), 1), head_size)
    diag = key_row == key_col
    count = counts[seq]
    for t in range(slots):

        @pl.when(t < count)
        def _():
            at = pl.ds(seq * slots + t, 1)
            for j in range(cols // tile):
                here = slice(j * tile, (j + 1) * tile)
                kq = jnp.concatenate(
                    [
                        jnp.where(diag, jnp.broadcast_to(k_s[at, here], (size, tile)), 0.0),
                        jnp.where(diag, jnp.broadcast_to(q_s[at, here], (size, tile)), 0.0),
                    ],
                    axis=0,
                ).astype(BF16)
                kq = jnp.dot(kq, blocks, preferred_element_type=F32)
                kmat, qmat = kq[:size], kq[size:]
                decayed = new[0, 0, :, here] * dec_s[at, here]
                guess = jnp.sum(decayed * kmat, axis=0, keepdims=True)
                fresh = beta_s[at, here] * (v_s[at, here] - guess)
                updated = decayed + kmat * fresh
                new[0, 0, :, here] = updated
                o_s[at, here] = jnp.sum(updated * qmat, axis=0, keepdims=True)

    @pl.when(seq == pl.num_programs(0) - 1)
    def _():
        own = q_s.shape[0]
        packed = main.shape[0]
        place = (lax.broadcasted_iota(jnp.int32, (packed, own), 0) == pos_row[...]).astype(BF16)
        for j in range(cols // tile):
            here = slice(j * tile, (j + 1) * tile)
            val = o_s[:, here]
            total = jnp.dot((val * val).astype(BF16), blocks, preferred_element_type=F32)
            val = val * lax.rsqrt(total / head_size + EPS) * gain[:, here] * z_s[:, here]
            y[:, here] = jnp.dot(place, val.astype(BF16), preferred_element_type=F32).astype(BF16)


def recur(counts, where, main, small, pos, speed, bias, shrink, gain, states, carried, layer, width, heads_all):
    own_seqs = counts.shape[0]
    packed = main.shape[0]
    size, cols = states.shape[2:]
    own = pos.shape[0]
    heads = speed.shape[1]
    whole = lambda shape: pl.BlockSpec(shape, lambda s, *_: (0,) * len(shape))
    here = pl.BlockSpec((1, 1, size, cols), lambda s, *_: (layer, s, 0, 0))
    args = [main, small, pos[:, None], pos[None, :], speed, bias, shrink, gain]
    specs = [whole(a.shape) for a in args] + [here]
    kernel = functools.partial(recur_kernel, width, size, cols // heads, heads_all)
    if carried is None:
        body = lambda *refs: kernel(*refs[:11], None, *refs[11:])
        more, alias = [], {}
    else:
        body = kernel
        more, alias = [carried], {11: 1}
        specs = specs + [pl.BlockSpec(memory_space=pl.ANY)]
    return pl.pallas_call(
        body,
        out_shape=[
            jax.ShapeDtypeStruct((packed, cols), BF16),
            jax.ShapeDtypeStruct(states.shape, F32),
        ],
        grid_spec=pltpu.PrefetchScalarGridSpec(
            num_scalar_prefetch=2,
            grid=(own_seqs,),
            in_specs=specs,
            out_specs=[whole((packed, cols)), here],
            scratch_shapes=[pltpu.VMEM((own, cols), F32) for _ in range(7)],
        ),
        input_output_aliases=alias,
        name="recur",
    )(counts, where, *args, states, *more)


def gated_kernel(n, y, out, *rest):
    reduce_over_dp(n, [y], [out], [rest[0:4]], rest[4:6])


def share_gated(y, n, cid):
    return pl.pallas_call(
        functools.partial(gated_kernel, n),
        out_shape=jax.ShapeDtypeStruct(y.shape, BF16),
        in_specs=[VMEM],
        out_specs=VMEM,
        scratch_shapes=reduce_scratch(n, [y.shape]),
        compiler_params=params(cid),
        name="share_gated",
    )(y)


def mix_kernel(m, gated, w, h, out, part, land, own, gath, send_a, recv_a, send_b, recv_b):
    me = lax.axis_index("tp")
    peers = [lax.rem(me + d, m) for d in range(1, m)]
    greet("tp", peers)
    rows = part.shape[1]
    mixed = jnp.dot(gated[...], w[0], preferred_element_type=F32)
    for j in range(m):
        part[j] = mixed[j * rows : (j + 1) * rows].astype(BF16)
    copies = [
        send(part.at[peer], land.at[d], send_a.at[d], recv_a.at[d], "tp", peer)
        for d, peer in enumerate(peers)
    ]
    total = part[me].astype(F32)
    for d, copy in enumerate(copies):
        copy.wait()
        total = total + land[d].astype(F32)
    own[...] = total.astype(BF16)
    copies = [
        send(own, gath.at[me], send_b.at[d], recv_b.at[d], "tp", peer)
        for d, peer in enumerate(peers)
    ]
    for copy in copies:
        copy.wait()
    gath[me] = own[...]
    for j in range(m):
        at = slice(j * rows, (j + 1) * rows)
        out[at, :] = (h[at, :] + gath[j].astype(F32)).astype(BF16).astype(F32)


def mix(gated, w, h, layer, m, cid):
    packed, feat = h.shape
    cols = gated.shape[1]
    rows = packed // m
    once = lambda shape: pl.BlockSpec(shape, lambda i: (0,) * len(shape))
    return pl.pallas_call(
        functools.partial(mix_kernel, m),
        grid=(1,),
        out_shape=jax.ShapeDtypeStruct(h.shape, F32),
        in_specs=[
            once(gated.shape),
            pl.BlockSpec((1, cols, feat), lambda i: (layer, 0, 0)),
            once(h.shape),
        ],
        out_specs=once(h.shape),
        scratch_shapes=[
            pltpu.VMEM((m, rows, feat), BF16),
            pltpu.VMEM((m - 1, rows, feat), BF16),
            pltpu.VMEM((rows, feat), BF16),
            pltpu.VMEM((m, rows, feat), BF16),
            *[pltpu.SemaphoreType.DMA((m - 1,)) for _ in range(4)],
        ],
        compiler_params=params(cid),
        name="mix",
    )(gated, w, h)


def body(
    n,
    m,
    resid,
    counts,
    wq,
    wk,
    wv,
    wz,
    wa,
    wb,
    wo,
    speed,
    bias,
    scaling,
    channel,
    shrink,
    states,
):
    all_seqs, slots, feat = resid.shape
    own_seqs = counts.shape[0]
    own = own_seqs * slots
    heads = speed.shape[1]
    live_rows = all_seqs * 3 // 2
    step = -(-live_rows // m)
    step = -(-step // 8) * 8
    while step * m % 32:
        step += 8
    packed = step * m
    dp = lax.axis_index("dp")
    where = jnp.stack([dp, lax.axis_index("tp")]).astype(jnp.int32)
    every = gather_counts(counts, n, 1)
    before = lax.broadcasted_iota(jnp.int32, (all_seqs, all_seqs), 1) < lax.broadcasted_iota(
        jnp.int32, (all_seqs, all_seqs), 0
    )
    start = jnp.sum(jnp.where(before, every[None, :], 0), axis=1)
    slot = lax.broadcasted_iota(jnp.int32, (all_seqs, slots), 1)
    pos = jnp.where(slot < every[:, None], start[:, None] + slot, -1).reshape(all_seqs * slots)
    pos_own = lax.dynamic_slice_in_dim(pos, dp * own, own, 0)
    onehot = (lax.broadcasted_iota(jnp.int32, (packed, all_seqs * slots), 0) == pos[None, :]).astype(BF16)
    flat = resid.reshape(all_seqs * slots, feat)
    h = jnp.dot(onehot, flat, preferred_element_type=F32)
    carried = None
    for l in range(BLOCKS):
        main, small = project(h, scaling[l][None], (wq, wk, wv, wz), wa, wb, l, where)
        main, small = sum_projections(main, small, n, 2 + 3 * l)
        gain = jnp.tile(channel[l].astype(F32), heads)[None]
        y, carried = recur(
            counts, where, main, small, pos_own, speed[l][None], bias[l][None],
            shrink[l].reshape(own, heads), gain, states, carried, l, feat * n, wa.shape[2],
        )
        gated = share_gated(y, n, 3 + 3 * l)
        h = mix(gated, wo, h, l, m, 4 + 3 * l)
    back = lax.dot_general(
        onehot, h.astype(BF16), (((0,), (0,)), ((), ())), preferred_element_type=F32
    )
    out = jnp.where(pos[:, None] >= 0, back, flat.astype(F32)).astype(BF16)
    return out.reshape(all_seqs, slots, feat), carried


def solution(mesh):
    in_specs = (
        P("grp", None, "dp"),
        P(("grp", "dp")),
        P(None, "dp", "tp"),
        P(None, "dp", "tp"),
        P(None, "dp", "tp"),
        P(None, "dp", "tp"),
        P(),
        P(),
        P(None, "tp", "dp"),
        P(None, "tp"),
        P(None, "tp"),
        P(None, "dp"),
        P(),
        P(None, ("grp", "dp"), None, "tp"),
        P(None, ("grp", "dp"), None, "tp"),
    )
    out_specs = (P("grp", None, "dp"), P(None, ("grp", "dp"), None, "tp"))
    run = functools.partial(body, mesh.shape["dp"], mesh.shape["tp"])
    return jax.shard_map(run, mesh=mesh, in_specs=in_specs, out_specs=out_specs, check_vma=False)
```

```python
import functools

import jax
import jax.numpy as jnp
from jax import lax
from jax.experimental import pallas as pl
from jax.experimental.pallas import tpu as pltpu
from jax.sharding import PartitionSpec as P

BLOCKS = 2
EPS = 1e-06
F32 = jnp.float32
BF16 = jnp.bfloat16
MESH = pl.DeviceIdType.MESH
VMEM = pl.BlockSpec(memory_space=pltpu.VMEM)


def greet(axis, peers):
    barrier = pltpu.get_barrier_semaphore()
    for peer in peers:
        pl.semaphore_signal(barrier, inc=1, device_id={axis: peer}, device_id_type=MESH)
    pl.semaphore_wait(barrier, len(peers))


def send(src, dst, send_sem, recv_sem, axis, peer):
    copy = pltpu.make_async_remote_copy(
        src_ref=src,
        dst_ref=dst,
        send_sem=send_sem,
        recv_sem=recv_sem,
        device_id={axis: peer},
        device_id_type=MESH,
    )
    copy.start()
    return copy


def params(cid):
    return pltpu.CompilerParams(
        collective_id=cid, has_side_effects=True, vmem_limit_bytes=48 * 1024 * 1024
    )


def gather_kernel(n, x_ref, o_ref, land, send_sem, recv_sem):
    me = lax.axis_index("dp")
    peers = [lax.rem(me + d, n) for d in range(1, n)]
    greet("dp", peers)
    copies = [
        send(x_ref, land.at[me], send_sem.at[d], recv_sem.at[d], "dp", peer)
        for d, peer in enumerate(peers)
    ]
    for copy in copies:
        copy.wait()
    o_ref[...] = land[...]
    o_ref[me] = x_ref[...]


def gather_counts(counts, n, cid):
    own = counts.shape[0]
    block = jnp.broadcast_to(jnp.pad(counts, (0, 128 - own))[None, :], (8, 128))
    out = pl.pallas_call(
        functools.partial(gather_kernel, n),
        out_shape=jax.ShapeDtypeStruct((n, 8, 128), jnp.int32),
        in_specs=[VMEM],
        out_specs=VMEM,
        scratch_shapes=[
            pltpu.VMEM((n, 8, 128), jnp.int32),
            pltpu.SemaphoreType.DMA((n - 1,)),
            pltpu.SemaphoreType.DMA((n - 1,)),
        ],
        compiler_params=params(cid),
        name="gather_counts",
    )(block)
    return out[:, 0, :own].reshape(n * own)


def dp_partners(n):
    me = lax.axis_index("dp")
    core = lax.rem(me, 2)
    partner = me + 1 - 2 * core
    return core, partner, [lax.rem(me + 2 * d, n) for d in range(1, n // 2)]


def reduce_over_dp(n, produce, x_refs, store, scratch, sems):
    chips = n // 2
    core, partner, others = dp_partners(n)
    send_sem, recv_sem = sems
    width = chips + 1
    rows = x_refs[0].shape[0] // 2
    mine = pl.multiple_of(core * rows, 16)
    theirs = pl.multiple_of((1 - core) * rows, 16)
    first, second, third = [], [], []

    def cross(a):
        x = x_refs[a]
        half, own, land, back = scratch[a]
        first[a].wait()
        for r in range(0, rows, 16):
            chunk = x[pl.ds(pl.multiple_of(mine + r, 16), 16), :].astype(F32) + half[pl.ds(r, 16), :].astype(F32)
            own[pl.ds(r, 16), :] = chunk.astype(BF16)
        second.append(
            [
                send(own, land.at[d], send_sem.at[a * width + 1 + d], recv_sem.at[a * width + 1 + d], "dp", peer)
                for d, peer in enumerate(others)
            ]
        )

    for a, x in enumerate(x_refs):
        produce(a)
        first.append(
            send(
                x.at[pl.ds(theirs, rows)], scratch[a][0], send_sem.at[a * width],
                recv_sem.at[a * width], "dp", partner,
            )
        )
        if a:
            cross(a - 1)
    cross(len(x_refs) - 1)
    for a in range(len(x_refs)):
        half, own, land, back = scratch[a]
        for copy in second[a]:
            copy.wait()
        for r in range(0, rows, 16):
            total = own[pl.ds(r, 16), :].astype(F32)
            for d in range(chips - 1):
                total = total + land[d, pl.ds(r, 16), :].astype(F32)
            own[pl.ds(r, 16), :] = total.astype(BF16)
        slot = a * width + chips
        third.append(send(own, back, send_sem.at[slot], recv_sem.at[slot], "dp", partner))
    for a in range(len(x_refs)):
        half, own, land, back = scratch[a]
        store(a, pl.ds(mine, rows), own[...])
        third[a].wait()
        store(a, pl.ds(theirs, rows), back[...])


def reduce_scratch(n, shapes):
    out = []
    for rows, cols in shapes:
        half = (rows // 2, cols)
        out += [
            pltpu.VMEM(half, BF16),
            pltpu.VMEM(half, BF16),
            pltpu.VMEM((n // 2 - 1,) + half, BF16),
            pltpu.VMEM(half, BF16),
        ]
    count = len(shapes) * (n // 2 + 1)
    return out + [pltpu.SemaphoreType.DMA((count,)), pltpu.SemaphoreType.DMA((count,))]


def proj_kernel(n, layer, h, gain, wab, wq, wk, wv, wz, main, small, wbuf, scaled, w_sem, *rest):
    feat, cols = wbuf.shape[1:]
    tile = min(256, cols)
    chunks = cols // tile
    loads = []
    for j in range(chunks):
        for i, w in enumerate((wq, wk, wv, wz)):
            at = pl.ds(j * tile, tile)
            load = pltpu.make_async_copy(w.at[layer, :, at], wbuf.at[i, :, at], w_sem.at[4 * j + i])
            load.start()
            loads.append(load)
    core, partner, others = dp_partners(n)
    greet("dp", [partner] + others)
    count = chunks + 1
    x_refs = rest[:count]
    scratch = [rest[count + 4 * a : count + 4 * a + 4] for a in range(count)]
    pair = wab.shape[2]

    def produce(a):
        x = x_refs[a]
        if a == 0:
            rows = h[...]
            bent = (rows * gain[...].astype(F32)).astype(BF16)
            scaled[...] = bent
            x[:, :pair] = jnp.dot(bent, wab[layer], preferred_element_type=F32).astype(BF16)
            squares = jnp.sum(rows * rows, axis=1, keepdims=True)
            x[:, pair:] = jnp.broadcast_to(squares, (rows.shape[0], x.shape[1] - pair)).astype(BF16)
            return
        j = a - 1
        for i in range(4):
            loads[4 * j + i].wait()
            x[:, i * tile : (i + 1) * tile] = jnp.dot(
                scaled[...], wbuf[i, :, j * tile : (j + 1) * tile], preferred_element_type=F32
            ).astype(BF16)

    def store(a, at, val):
        if a == 0:
            small[at, :] = val
        else:
            main[at, (a - 1) * 4 * tile : a * 4 * tile] = val

    reduce_over_dp(n, produce, x_refs, store, scratch, rest[-2:])


def project(h, gain, weights, wab, layer, n, cid):
    rows, feat = h.shape
    cols = weights[0].shape[2]
    tile = min(256, cols)
    chunks = cols // tile
    shapes = [(rows, wab.shape[2] + 128)] + [(rows, 4 * tile)] * chunks
    return pl.pallas_call(
        functools.partial(proj_kernel, n, layer),
        out_shape=[
            jax.ShapeDtypeStruct((rows, 4 * cols), BF16),
            jax.ShapeDtypeStruct(shapes[0], BF16),
        ],
        in_specs=[VMEM, VMEM, VMEM] + [pl.BlockSpec(memory_space=pl.ANY)] * 4,
        out_specs=[VMEM, VMEM],
        scratch_shapes=[
            pltpu.VMEM((4, feat, cols), BF16),
            pltpu.VMEM((rows, feat), BF16),
            pltpu.SemaphoreType.DMA((4 * chunks,)),
            *[pltpu.VMEM(shape, BF16) for shape in shapes],
            *reduce_scratch(n, shapes),
        ],
        compiler_params=params(cid),
        name="project",
    )(h, gain, wab, *weights)


def recur_kernel(
    width, size, head_size, heads_all, counts, where, main, small, pos_col, pos_row, speed, bias,
    shrink, gain, state, carried, y, new, q_s, k_s, v_s, z_s, dec_s, beta_s, o_s,
):
    group = state.shape[1]
    slots = q_s.shape[0] // (pl.num_programs(0) * group)
    tile = min(256, q_s.shape[1])
    cols = q_s.shape[1]
    row = lax.broadcasted_iota(jnp.int32, (tile, tile), 0) // head_size
    col = lax.broadcasted_iota(jnp.int32, (tile, tile), 1) // head_size
    blocks = (row == col).astype(BF16)

    @pl.when(pl.program_id(0) == 0)
    def _():
        own = q_s.shape[0]
        packed = main.shape[0]
        pick = (pos_col[...] == lax.broadcasted_iota(jnp.int32, (own, packed), 1)).astype(BF16)
        few = jnp.dot(pick, small[...], preferred_element_type=F32)
        factor = lax.rsqrt(few[:, 2 * heads_all : 2 * heads_all + 1] / width + EPS)
        heads = speed.shape[1]
        first = where[1] * heads
        ones = lax.broadcasted_iota(jnp.int32, (heads_all, cols), 0)
        lane = lax.broadcasted_iota(jnp.int32, (heads_all, cols), 1) // head_size
        spread_all = (ones == lane + first).astype(BF16)
        spread = (
            lax.broadcasted_iota(jnp.int32, (heads, cols), 0)
            == lax.broadcasted_iota(jnp.int32, (heads, cols), 1) // head_size
        ).astype(F32)
        pa = jnp.dot(few[:, :heads_all].astype(BF16), spread_all, preferred_element_type=F32) * factor
        pb = jnp.dot(
            few[:, heads_all : 2 * heads_all].astype(BF16), spread_all, preferred_element_type=F32
        ) * factor
        exact = functools.partial(
            jnp.dot, precision=lax.Precision.HIGHEST, preferred_element_type=F32
        )
        rate = exact(jnp.broadcast_to(jnp.exp(speed[...]), (8, heads)), spread)[:1]
        offset = exact(jnp.broadcast_to(bias[...], (8, heads)), spread)[:1]
        extra = exact(shrink[...], spread)
        arg = pa + offset
        soft = jnp.maximum(arg, 0.0) + jnp.log1p(jnp.exp(-jnp.abs(arg)))
        dec_s[...] = jnp.exp(extra - rate * soft)
        beta_s[...] = jax.nn.sigmoid(pb)
        for j in range(cols // tile):
            here = slice(j * tile, (j + 1) * tile)
            chunk = jnp.dot(
                pick, main[:, j * 4 * tile : (j + 1) * 4 * tile], preferred_element_type=F32
            ) * factor
            for i, dst in enumerate((q_s, k_s, v_s, z_s)):
                val = chunk[:, i * tile : (i + 1) * tile]
                val = val * jax.nn.sigmoid(val)
                if i < 2:
                    total = jnp.dot((val * val).astype(BF16), blocks, preferred_element_type=F32)
                    val = val * lax.rsqrt(total + EPS)
                    if i == 0:
                        val = val * head_size ** (-0.5)
                dst[:, here] = val
        o_s[...] = jnp.zeros_like(o_s)

    new[...] = state[...]
    key_row = lax.broadcasted_iota(jnp.int32, (size, tile), 0)
    key_col = lax.rem(lax.broadcasted_iota(jnp.int32, (size, tile), 1), head_size)
    diag = key_row == key_col
    for g in range(group):
        seq = pl.program_id(0) * group + g
        for t in range(slots):

            @pl.when(t < counts[seq])
            def _():
                at = pl.ds(seq * slots + t, 1)
                for j in range(cols // tile):
                    here = slice(j * tile, (j + 1) * tile)
                    kq = jnp.concatenate(
                        [
                            jnp.where(diag, jnp.broadcast_to(k_s[at, here], (size, tile)), 0.0),
                            jnp.where(diag, jnp.broadcast_to(q_s[at, here], (size, tile)), 0.0),
                        ],
                        axis=0,
                    ).astype(BF16)
                    kq = jnp.dot(kq, blocks, preferred_element_type=F32)
                    kmat, qmat = kq[:size], kq[size:]
                    decayed = new[0, g, :, here] * dec_s[at, here]
                    guess = jnp.sum(decayed * kmat, axis=0, keepdims=True)
                    fresh = beta_s[at, here] * (v_s[at, here] - guess)
                    updated = decayed + kmat * fresh
                    new[0, g, :, here] = updated
                    o_s[at, here] = jnp.sum(updated * qmat, axis=0, keepdims=True)

    @pl.when(pl.program_id(0) == pl.num_programs(0) - 1)
    def _():
        own = q_s.shape[0]
        packed = main.shape[0]
        place = (lax.broadcasted_iota(jnp.int32, (packed, own), 0) == pos_row[...]).astype(BF16)
        for j in range(cols // tile):
            here = slice(j * tile, (j + 1) * tile)
            val = o_s[:, here]
            total = jnp.dot((val * val).astype(BF16), blocks, preferred_element_type=F32)
            val = val * lax.rsqrt(total / head_size + EPS) * gain[:, here] * z_s[:, here]
            y[:, here] = jnp.dot(place, val.astype(BF16), preferred_element_type=F32).astype(BF16)


def recur(counts, where, main, small, pos, speed, bias, shrink, gain, states, carried, layer, width, heads_all):
    own_seqs = counts.shape[0]
    group = 2 if own_seqs % 2 == 0 else 1
    packed = main.shape[0]
    size, cols = states.shape[2:]
    own = pos.shape[0]
    heads = speed.shape[1]
    whole = lambda shape: pl.BlockSpec(shape, lambda s, *_: (0,) * len(shape))
    here = pl.BlockSpec((1, group, size, cols), lambda s, *_: (layer, s, 0, 0))
    args = [main, small, pos[:, None], pos[None, :], speed, bias, shrink, gain]
    specs = [whole(a.shape) for a in args] + [here]
    kernel = functools.partial(recur_kernel, width, size, cols // heads, heads_all)
    if carried is None:
        body = lambda *refs: kernel(*refs[:11], None, *refs[11:])
        more, alias = [], {}
    else:
        body = kernel
        more, alias = [carried], {11: 1}
        specs = specs + [pl.BlockSpec(memory_space=pl.ANY)]
    return pl.pallas_call(
        body,
        out_shape=[
            jax.ShapeDtypeStruct((packed, cols), BF16),
            jax.ShapeDtypeStruct(states.shape, F32),
        ],
        grid_spec=pltpu.PrefetchScalarGridSpec(
            num_scalar_prefetch=2,
            grid=(own_seqs // group,),
            in_specs=specs,
            out_specs=[whole((packed, cols)), here],
            scratch_shapes=[pltpu.VMEM((own, cols), F32) for _ in range(7)],
        ),
        input_output_aliases=alias,
        name="recur",
    )(counts, where, *args, states, *more)


def mix_kernel(
    n, m, layer, y, w, h, out, wbuf, w_sem, gated, part, land, own, gath,
    send_a, recv_a, send_b, recv_b, *rest,
):
    load = pltpu.make_async_copy(w.at[layer], wbuf, w_sem)
    load.start()
    me = lax.axis_index("tp")
    peers = [lax.rem(me + d, m) for d in range(1, m)]
    core, partner, others = dp_partners(n)
    barrier = pltpu.get_barrier_semaphore()
    for axis, group in (("dp", [partner] + others), ("tp", peers)):
        for peer in group:
            pl.semaphore_signal(barrier, inc=1, device_id={axis: peer}, device_id_type=MESH)
    pl.semaphore_wait(barrier, 1 + len(others) + len(peers))

    def store(a, at, val):
        gated[at, :] = val

    reduce_over_dp(n, lambda a: None, [y], store, [rest[0:4]], rest[4:6])
    load.wait()
    rows = part.shape[1]
    mixed = jnp.dot(gated[...], wbuf[...], preferred_element_type=F32)
    for j in range(m):
        part[j] = mixed[j * rows : (j + 1) * rows].astype(BF16)
    copies = [
        send(part.at[peer], land.at[d], send_a.at[d], recv_a.at[d], "tp", peer)
        for d, peer in enumerate(peers)
    ]
    total = part[me].astype(F32)
    for d, copy in enumerate(copies):
        copy.wait()
        total = total + land[d].astype(F32)
    own[...] = total.astype(BF16)
    copies = [
        send(own, gath.at[me], send_b.at[d], recv_b.at[d], "tp", peer)
        for d, peer in enumerate(peers)
    ]
    for copy in copies:
        copy.wait()
    gath[me] = own[...]
    for j in range(m):
        at = slice(j * rows, (j + 1) * rows)
        out[at, :] = (h[at, :] + gath[j].astype(F32)).astype(BF16).astype(F32)


def mix(y, w, h, layer, n, m, cid):
    packed, feat = h.shape
    rows = packed // m
    return pl.pallas_call(
        functools.partial(mix_kernel, n, m, layer),
        out_shape=jax.ShapeDtypeStruct(h.shape, F32),
        in_specs=[VMEM, pl.BlockSpec(memory_space=pl.ANY), VMEM],
        out_specs=VMEM,
        scratch_shapes=[
            pltpu.VMEM(w.shape[1:], BF16),
            pltpu.SemaphoreType.DMA,
            pltpu.VMEM(y.shape, BF16),
            pltpu.VMEM((m, rows, feat), BF16),
            pltpu.VMEM((m - 1, rows, feat), BF16),
            pltpu.VMEM((rows, feat), BF16),
            pltpu.VMEM((m, rows, feat), BF16),
            *[pltpu.SemaphoreType.DMA((m - 1,)) for _ in range(4)],
            *reduce_scratch(n, [y.shape]),
        ],
        compiler_params=params(cid),
        name="mix",
    )(y, w, h)


def body(
    n,
    m,
    resid,
    counts,
    wq,
    wk,
    wv,
    wz,
    wa,
    wb,
    wo,
    speed,
    bias,
    scaling,
    channel,
    shrink,
    states,
):
    all_seqs, slots, feat = resid.shape
    own_seqs = counts.shape[0]
    own = own_seqs * slots
    heads = speed.shape[1]
    live_rows = all_seqs * 3 // 2
    step = -(-live_rows // m)
    step = -(-step // 8) * 8
    while step * m % 32:
        step += 8
    packed = step * m
    dp = lax.axis_index("dp")
    where = jnp.stack([dp, lax.axis_index("tp")]).astype(jnp.int32)
    every = gather_counts(counts, n, 1)
    cut = lambda w: lax.dynamic_slice_in_dim(w, dp * feat, feat, 1)
    wab = jnp.concatenate([cut(wa), cut(wb)], axis=2)
    before = lax.broadcasted_iota(jnp.int32, (all_seqs, all_seqs), 1) < lax.broadcasted_iota(
        jnp.int32, (all_seqs, all_seqs), 0
    )
    start = jnp.sum(jnp.where(before, every[None, :], 0), axis=1)
    slot = lax.broadcasted_iota(jnp.int32, (all_seqs, slots), 1)
    pos = jnp.where(slot < every[:, None], start[:, None] + slot, -1).reshape(all_seqs * slots)
    pos_own = lax.dynamic_slice_in_dim(pos, dp * own, own, 0)
    onehot = (lax.broadcasted_iota(jnp.int32, (packed, all_seqs * slots), 0) == pos[None, :]).astype(BF16)
    flat = resid.reshape(all_seqs * slots, feat)
    h = jnp.dot(onehot, flat, preferred_element_type=F32)
    carried = None
    for l in range(BLOCKS):
        main, small = project(h, scaling[l][None], (wq, wk, wv, wz), wab, l, n, 2 + 2 * l)
        gain = jnp.tile(channel[l].astype(F32), heads)[None]
        y, carried = recur(
            counts, where, main, small, pos_own, speed[l][None], bias[l][None],
            shrink[l].reshape(own, heads), gain, states, carried, l, feat * n, wa.shape[2],
        )
        h = mix(y, wo, h, l, n, m, 3 + 2 * l)
    back = lax.dot_general(
        onehot, h.astype(BF16), (((0,), (0,)), ((), ())), preferred_element_type=F32
    )
    out = jnp.where(pos[:, None] >= 0, back, flat.astype(F32)).astype(BF16)
    return out.reshape(all_seqs, slots, feat), carried


def solution(mesh):
    in_specs = (
        P("grp", None, "dp"),
        P(("grp", "dp")),
        P(None, "dp", "tp"),
        P(None, "dp", "tp"),
        P(None, "dp", "tp"),
        P(None, "dp", "tp"),
        P(),
        P(),
        P(None, "tp", "dp"),
        P(None, "tp"),
        P(None, "tp"),
        P(None, "dp"),
        P(),
        P(None, ("grp", "dp"), None, "tp"),
        P(None, ("grp", "dp"), None, "tp"),
    )
    out_specs = (P("grp", None, "dp"), P(None, ("grp", "dp"), None, "tp"))
    run = functools.partial(body, mesh.shape["dp"], mesh.shape["tp"])
    return jax.shard_map(run, mesh=mesh, in_specs=in_specs, out_specs=out_specs, check_vma=False)
```
